32 devices in a mesh: sp: 8 (over z, y), tp: 4 (over x, core).
Axes of the slice: x: 2, y: 2, z: 4, core: 2. Of those that a mesh axis runs over, the one named last changes fastest.
Arguments:
- tokens: bfloat16 [2048, 1024], P(('sp', 'tp')), may hold values from -7.5 to 7.5, as said below
- query_weight: bfloat16 [1024, 2048], P('sp', 'tp'), may hold values from -0.1875 to 0.1875
- key_weight: bfloat16 [1024, 2048], P('sp', 'tp'), may hold values from -0.1875 to 0.1875
- value_weight: bfloat16 [1024, 2048], P('sp', 'tp'), may hold values from -0.1875 to 0.1875
- gate_weight: bfloat16 [1024, 16], P('sp', 'tp'), may hold values from -0.1875 to 0.1875
- forget_bias: float32 [16], P('tp'), may hold values from 0 to 2
- out_weight: bfloat16 [2048, 1024], P('tp', 'sp'), may hold values from -0.125 to 0.125
- out_gain: float32 [1024], replicated, may hold values from 0.5 to 1.5
Outputs:
- mixed: bfloat16 [2048, 1024], P(('sp', 'tp'))
The draws below stay inside these ranges and needn't reach their ends.
Inputs may be any that keep to these rules, and one draw needn't show every extreme that they name: `tokens`: each entry is a bounded noise value (at most 6 in size) plus an offset in -1.5 to 1.5 shared by the 256 rows of one index of sp, so every entry lies within -7.5 and 7.5.
All inputs are finite; a program needn't handle non-finite values.
Results may differ from the reference program's by a relative error of at most 0.006.
Values may be sent and summed in bfloat16 or wider, within the bound.
A program may use at most 128 MiB of HBM per device.

```python
import math
import jax
import jax.numpy as jnp
from jax import lax

D = 1024
HEADS = 16
HEAD_DIM = 128
TOK_DEV = 256
WIDTH = 2048
SEQ = 2048


def draw_tokens(key, part):
    noise_key = jax.random.fold_in(key, 11)
    shift_key = jax.random.fold_in(key, 12)
    noise = jax.random.truncated_normal(noise_key, -6.0, 6.0, (SEQ, D), jnp.float32)
    shifts = jax.random.uniform(shift_key, (SEQ // TOK_DEV, D), jnp.float32, -1.5, 1.5)
    return (noise + jnp.repeat(shifts, TOK_DEV, axis=0)).astype(jnp.bfloat16)


def block_scale(stream_key, extent, cuts, low, top_value):
    level = 1.0
    for dim, shards_of in cuts:
        draws = jax.random.uniform(jax.random.fold_in(jax.random.fold_in(stream_key, 6), dim), (shards_of,), jnp.float32, low / len(cuts), top_value / len(cuts))
        level = level * jnp.repeat(jnp.exp(draws), extent[dim] // shards_of).reshape((-1,) + (1,) * (len(extent) - 1 - dim))
    return level


def gaussian(own_key, dims, width, most, cuts=(), kind=jnp.bfloat16):
    factor_of = block_scale(own_key, dims, cuts, -0.22, 0.18) if cuts else 1.0
    values = jax.random.normal(own_key, dims, jnp.float32) * width * factor_of
    return jnp.minimum(jnp.maximum(values, -most), most).astype(kind)


def setup_inputs(seed: int = 0) -> dict:
    key_of = jax.random.split(jax.random.key(seed), 9)
    tokens = draw_tokens(jax.random.fold_in(key_of[8], 71), 0)
    query_weight = gaussian(key_of[1], (D, WIDTH), D ** -0.5, 0.1875, ((0, 8), (1, 4)))
    key_weight = gaussian(key_of[2], (D, WIDTH), D ** -0.5, 0.1875, ((0, 8), (1, 4)))
    value_weight = gaussian(key_of[3], (D, WIDTH), D ** -0.5, 0.1875, ((0, 8), (1, 4)))
    gate_weight = gaussian(key_of[4], (D, HEADS), D ** -0.5, 0.1875, ((0, 8), (1, 4)))
    forget_bias = jnp.clip(2.0 * jax.random.uniform(key_of[5], (HEADS,), jnp.float32) ** block_scale(key_of[5], (HEADS,), ((0, 4),), -0.2, 0.2), 0.0, 2.0)
    out_weight = gaussian(key_of[6], (WIDTH, D), WIDTH ** -0.5, 0.125, ((0, 4), (1, 8)))
    out_gain = jnp.clip(1.0 + 0.1 * jax.random.normal(key_of[7], (D,), jnp.float32), 0.5, 1.5)
    return {"tokens": tokens, "query_weight": query_weight, "key_weight": key_weight, "value_weight": value_weight, "gate_weight": gate_weight, "forget_bias": forget_bias, "out_weight": out_weight, "out_gain": out_gain}


def reference(tokens, query_weight, key_weight, value_weight, gate_weight, forget_bias, out_weight, out_gain):
    queries = jnp.dot(tokens, query_weight, preferred_element_type=jnp.float32).astype(jnp.bfloat16)
    keys = jnp.dot(tokens, key_weight, preferred_element_type=jnp.float32).astype(jnp.bfloat16)
    values = jnp.dot(tokens, value_weight, preferred_element_type=jnp.float32).astype(jnp.bfloat16)
    queries = queries.reshape(SEQ, HEADS, HEAD_DIM).astype(jnp.float32)
    keys = keys.reshape(SEQ, HEADS, HEAD_DIM).astype(jnp.float32)
    values = values.reshape(SEQ, HEADS, HEAD_DIM).astype(jnp.float32)
    raw_gate = jnp.dot(tokens, gate_weight, preferred_element_type=jnp.float32)
    log_gate = jax.nn.log_sigmoid(raw_gate + forget_bias + math.log(SEQ))
    cumulative = jnp.cumsum(log_gate, axis=0)
    scale = HEAD_DIM ** (-0.5)
    key_pos = jnp.arange(SEQ, dtype=jnp.int32)

    def one_block(index):
        start = (index * TOK_DEV).astype(jnp.int32)
        block_q = lax.dynamic_slice_in_dim(queries, start, TOK_DEV, 0)
        block_c = lax.dynamic_slice_in_dim(cumulative, start, TOK_DEV, 0)
        logits = jnp.einsum('qhd,khd->hqk', block_q, keys) * scale
        logits = logits + block_c.T[:, :, None] - cumulative.T[:, None, :]
        query_pos = start + jnp.arange(TOK_DEV, dtype=jnp.int32)
        allowed = key_pos[None, :] <= query_pos[:, None]
        logits = jnp.where(allowed[None], logits, -1e+30)
        weights = jax.nn.softmax(logits, axis=-1)
        result = jnp.einsum('hqk,khd->qhd', weights, values)
        return result.reshape(TOK_DEV, WIDTH).astype(jnp.bfloat16)
    attended = lax.map(one_block, jnp.arange(SEQ // TOK_DEV, dtype=jnp.int32)).reshape(SEQ, WIDTH)
    summed = jnp.dot(attended, out_weight, preferred_element_type=jnp.float32)
    normed = summed * lax.rsqrt(lax.optimization_barrier(jnp.mean(summed * summed, axis=-1, keepdims=True)) + 1e-06)
    return (normed * out_gain).astype(jnp.bfloat16)
```

```python
import math

import jax
import jax.numpy as jnp
from jax import lax
from jax.experimental import pallas as pl
from jax.experimental.pallas import tpu as pltpu
from jax.sharding import PartitionSpec as P


def on_whole(shard, axis, dim, block):
    whole = lax.all_gather(shard, axis, axis=dim, tiled=True)
    return block(whole, jnp.int32(0))


def over_all(shard, axis, dim, absorb, state):
    everything = jax.tree.map(lambda a: lax.all_gather(a, axis, axis=dim, tiled=True), shard)
    return absorb(state, everything, jnp.int32(0))


def own_rows(product, width, axis):
    everything = product(jnp.int32(0), lax.axis_size(axis) * width)
    own = lax.psum_scatter(everything, axis, scatter_dimension=0, tiled=True)
    return own


def on_device(
    tokens, query_weight, key_weight, value_weight, gate_weight, forget_bias, out_weight, out_gain
):
    width = query_weight.shape[1]
    heads = gate_weight.shape[1]
    head_size = width // heads
    whole_q = lax.all_gather(query_weight, "sp", axis=0, tiled=True)
    whole_k = lax.all_gather(key_weight, "sp", axis=0, tiled=True)
    whole_v = lax.all_gather(value_weight, "sp", axis=0, tiled=True)
    whole_g = lax.all_gather(gate_weight, "sp", axis=0, tiled=True)
    joined = jnp.concatenate([whole_q, whole_k, whole_v, whole_g], axis=1)

    def project(piece, start):
        return jnp.dot(piece, joined, preferred_element_type=jnp.float32)

    projected = on_whole(tokens, "tp", 0, project)
    block = projected.shape[0]
    queries = projected[:, :width].astype(jnp.bfloat16).reshape(block, heads, head_size)
    keys = projected[:, width : 2 * width].astype(jnp.bfloat16).reshape(block, heads, head_size)
    values = (
        projected[:, 2 * width : 3 * width].astype(jnp.bfloat16).reshape(block, heads, head_size)
    )
    seq_len = block * lax.axis_size("sp")
    log_gate = jax.nn.log_sigmoid(projected[:, 3 * width :] + forget_bias + math.log(seq_len))
    gates_all = lax.all_gather(log_gate, "sp", axis=0, tiled=True)
    cumulative = jnp.cumsum(gates_all, axis=0)
    first = lax.axis_index("sp") * block
    query_cum = lax.dynamic_slice_in_dim(cumulative, first, block, 0)
    query_pos = first + jnp.arange(block, dtype=jnp.int32)
    scale = head_size ** (-0.5)

    def update(carry, piece, start):
        run_max, run_sum, run_acc = carry
        key_piece, value_piece = piece
        length = key_piece.shape[0]
        key_cum = lax.dynamic_slice_in_dim(cumulative, start, length, 0)
        logits = (
            jnp.einsum("qhd,khd->hqk", queries, key_piece, preferred_element_type=jnp.float32)
            * scale
        )
        logits = logits + query_cum.T[:, :, None] - key_cum.T[:, None, :]
        key_pos = start + jnp.arange(length, dtype=jnp.int32)
        allowed = (key_pos[None, :] <= query_pos[:, None])[None]
        logits = jnp.where(allowed, logits, -1e30)
        new_max = jnp.maximum(run_max, jnp.max(logits, axis=-1))
        probs = jnp.where(allowed, jnp.exp(logits - new_max[..., None]), 0.0)
        factor = jnp.exp(run_max - new_max)
        new_sum = run_sum * factor + jnp.sum(probs, axis=-1)
        new_acc = run_acc * factor[..., None] + jnp.einsum(
            "hqk,khd->hqd", probs, value_piece.astype(jnp.float32)
        )
        return (new_max, new_sum, new_acc)

    def attend(carry, piece, start):
        return lax.cond(
            start > first + block - 1,
            lambda state: state,
            lambda state: update(state, piece, start),
            carry,
        )

    initial = (
        jnp.full((heads, block), -1e30, jnp.float32),
        jnp.zeros((heads, block), jnp.float32),
        jnp.zeros((heads, block, head_size), jnp.float32),
    )
    run_max, run_sum, run_acc = over_all((keys, values), "sp", 0, attend, initial)
    attended = (
        (run_acc / run_sum[..., None]).transpose(1, 0, 2).reshape(block, width).astype(jnp.bfloat16)
    )
    out_full = lax.all_gather(out_weight, "sp", axis=1, tiled=True)
    rows = tokens.shape[0]

    def term(start, count):
        return jnp.dot(
            lax.dynamic_slice_in_dim(attended, start, count, 0),
            out_full,
            preferred_element_type=jnp.float32,
        )

    summed = own_rows(term, rows, "tp")
    normed = summed * lax.rsqrt(jnp.mean(summed * summed, axis=-1, keepdims=True) + 1e-06)
    return (normed * out_gain).astype(jnp.bfloat16)


MESH = pl.DeviceIdType.MESH
Z_, X_, Y_, DA, DB, PC, PX, PY, PA, PB = range(10)


def rdma(src, dst, send, recv, sp, tp):
    return pltpu.make_async_remote_copy(
        src_ref=src,
        dst_ref=dst,
        send_sem=send,
        recv_sem=recv,
        device_id={"sp": sp, "tp": tp},
        device_id_type=MESH,
    )


class Place:
    def __init__(self, depth):
        sp, tp = lax.axis_index("sp"), lax.axis_index("tp")
        self.depth, self.sp, self.tp = depth, sp, tp
        self.z, self.y = sp // 2, lax.rem(sp, 2)
        self.x, self.c = tp // 2, lax.rem(tp, 2)

    def back(self, j):
        return lax.rem(self.z + self.depth - j, self.depth)

    def ahead(self, j):
        return lax.rem(self.z + j, self.depth)


class Gather:
    def __init__(self, at, own, buf, send, recv, local):
        self.at, self.own, self.buf = at, own, buf
        self.send, self.recv, self.local = send, recv, local
        self.rows = own.shape[0]
        self.sent = []

    def block(self, z, y, x, c, half=None):
        start = (((z * 2 + y) * 2 + x) * 2 + c) * self.rows
        size = self.rows
        if half is not None:
            size = self.rows // 2
            start = start + half * size
        return self.buf.at[pl.ds(pl.multiple_of(start, size), size)]

    def go(self, kind, j, dst, sp, tp, src=None):
        copy = rdma(
            dst if src is None else src,
            dst,
            self.send.at[kind, j],
            self.recv.at[kind, j],
            sp,
            tp,
        )
        copy.start()
        self.sent.append(copy)

    def arrived(self, kind, j, ref):
        pltpu.make_async_copy(ref, ref, self.recv.at[kind, j]).wait()

    def to_x(self, kind, j, ref, src=None):
        a = self.at
        self.go(kind, j, ref, a.sp, (1 - a.x) * 2 + a.c, src)

    def to_y(self, kind, j, ref, src=None):
        a = self.at
        self.go(kind, j, ref, a.z * 2 + 1 - a.y, a.tp, src)

    def to_core(self, kind, j, ref, src=None):
        a = self.at
        self.go(kind, j, ref, a.sp, a.x * 2 + 1 - a.c, src)

    def begin(self):
        a = self.at
        mine = self.block(a.z, a.y, a.x, a.c)
        self.keep = pltpu.make_async_copy(self.own, mine, self.local)
        self.keep.start()
        self.to_x(X_, 0, mine, self.own)
        self.to_y(Y_, 0, mine, self.own)
        for j in range(1, a.depth):
            self.go(Z_, j, mine, a.ahead(j) * 2 + a.y, a.tp, self.own)
        self.to_core(PC, 0, mine, self.own)

    def column(self, j):
        a = self.at
        ref = self.block(a.back(j), a.y, a.x, a.c)
        self.arrived(Z_, j, ref)
        self.to_x(X_, j, ref)
        self.to_y(Y_, j, ref)
        self.to_core(PC, j, ref)

    def sides(self, j):
        a = self.at
        z = a.back(j)
        ref = self.block(z, a.y, 1 - a.x, a.c)
        self.arrived(X_, j, ref)
        self.to_y(DA, j, self.block(z, a.y, 1 - a.x, a.c, 0))
        self.to_core(PX, j, ref)
        ref = self.block(z, 1 - a.y, a.x, a.c)
        self.arrived(Y_, j, ref)
        self.to_x(DB, j, self.block(z, 1 - a.y, a.x, a.c, 1))
        self.to_core(PY, j, ref)

    def corner(self, j):
        a = self.at
        z = a.back(j)
        for kind, onward, half in ((DA, PA, 0), (DB, PB, 1)):
            ref = self.block(z, 1 - a.y, 1 - a.x, a.c, half)
            self.arrived(kind, j, ref)
            self.to_core(onward, j, ref)

    def partner(self, j):
        a = self.at
        z, c = a.back(j), 1 - a.c
        self.arrived(PC, j, self.block(z, a.y, a.x, c))
        self.arrived(PX, j, self.block(z, a.y, 1 - a.x, c))
        self.arrived(PY, j, self.block(z, 1 - a.y, a.x, c))
        self.arrived(PA, j, self.block(z, 1 - a.y, 1 - a.x, c, 0))
        self.arrived(PB, j, self.block(z, 1 - a.y, 1 - a.x, c, 1))

    def end(self):
        self.keep.wait()
        for copy in self.sent:
            copy.wait_send()


def layer(
    depth, size, tok_ref, q_ref, k_ref, v_ref, g_ref, b_ref, ow_ref, gain_ref, out_ref,
    toks, outw, wq, wkv, gates, bias, keys, vals, cums, cumc, mine, att,
    tok_send, tok_recv, ow_send, ow_recv, w_send, w_recv, p_send, p_recv, a_send, a_recv, keep,
):
    at = Place(depth)
    z, y, x, c = at.z, at.y, at.x, at.c
    home = y == c
    seq = toks.shape[0]
    heads = 4 * depth
    rows = q_ref.shape[0]
    tok = Gather(at, tok_ref, toks, tok_send, tok_recv, keep.at[0])
    ow = Gather(at, ow_ref, outw, ow_send, ow_recv, keep.at[1])

    def w_parts(head, row_block):
        cols = pl.ds(pl.multiple_of(head * size, size), size)
        place = pl.ds(pl.multiple_of(row_block * rows, rows), rows)
        return (
            (q_ref.at[:, cols], wq.at[place]),
            (k_ref.at[:, cols], wkv.at[place, pl.ds(0, size)]),
            (v_ref.at[:, cols], wkv.at[place, pl.ds(size, size)]),
            (g_ref, gates.at[:, place]),
        )

    away = jnp.where(home, 0, 1)

    def send_w(j):
        head = at.ahead(j)
        return [
            rdma(a, b, w_send.at[i, j], w_recv.at[i, j, away], head * 2 + c, at.tp)
            for i, (a, b) in enumerate(w_parts(head, at.sp))
        ]

    def keep_w():
        return [
            pltpu.make_async_copy(a, b, w_recv.at[i, 0, 0])
            for i, (a, b) in enumerate(w_parts(z, at.sp))
        ]

    def pass_w():
        whole = ((wq, wq), (wkv, wkv), (gates, gates), (b_ref, bias))
        return [
            rdma(a, b, p_send.at[i], p_recv.at[i], at.sp, x * 2 + 1 - c)
            for i, (a, b) in enumerate(whole)
        ]

    tok.begin()
    for j in range(1, depth):
        for copy in send_w(j):
            copy.start()

    @pl.when(home)
    def _():
        for copy in keep_w():
            copy.start()

    @pl.when(jnp.logical_not(home))
    def _():
        for copy in send_w(0):
            copy.start()

    tok.sides(0)
    for j in range(1, depth):
        tok.column(j)
    ow.begin()
    for j in range(1, depth):
        tok.sides(j)
    for j in range(depth):
        tok.corner(j)

    @pl.when(home)
    def _():
        for j in range(depth):
            for e in range(2):
                for i, (_a, b) in enumerate(w_parts(z, at.back(j) * 2 + (y if e == 0 else 1 - y))):
                    pltpu.make_async_copy(b, b, w_recv.at[i, j, e]).wait()
        for copy in pass_w():
            copy.start()
        moved = pltpu.make_async_copy(b_ref, bias, keep.at[2])
        moved.start()
        moved.wait()

    tok.keep.wait()
    for j in range(depth):
        tok.partner(j)
    ow.sides(0)
    for j in range(1, depth):
        ow.column(j)

    @pl.when(jnp.logical_not(home))
    def _():
        for i, ref in enumerate((wq, wkv, gates, bias)):
            pltpu.make_async_copy(ref, ref, p_recv.at[i]).wait()

    raw = lax.dot_general(
        gates[...], toks[...], (((1,), (1,)), ((), ())), preferred_element_type=jnp.float32
    )[:8]
    raw = raw + bias[:, :1] + math.log(seq)
    run = jnp.minimum(raw, 0.0) - jnp.log1p(jnp.exp(-jnp.abs(raw)))
    lane = lax.broadcasted_iota(jnp.int32, run.shape, 1)
    step = 1
    while step < seq:
        run = run + jnp.where(lane >= step, pltpu.roll(run, step, 1), 0.0)
        step *= 2
    which = lax.broadcasted_iota(jnp.int32, run.shape, 0)
    chosen = jnp.sum(jnp.where(which == z, run, 0.0), axis=0, keepdims=True)
    cums[...] = jnp.broadcast_to(chosen, cums.shape)
    cumc[...] = jnp.broadcast_to(chosen, (128, seq)).T

    span = seq // (2 * depth)
    for i in range(2 * depth):
        part = pl.ds(i * span, span)
        both = jnp.dot(toks[part, :], wkv[...], preferred_element_type=jnp.float32)
        keys[part, :] = both[:, :size].astype(jnp.bfloat16)
        vals[part, :] = both[:, size:].astype(jnp.bfloat16)
    for j in range(1, depth):
        ow.sides(j)

    scale = size ** (-0.5)
    own = span // 4
    head = (2 * x + y) * depth + z

    def deliver(j, dx, dc, local):
        xx = x if dx == 0 else 1 - x
        cc = c if dc == 0 else 1 - c
        start = pl.multiple_of(j * span + (xx * 2 + cc) * own, own)
        src = mine.at[pl.ds(start, own)]
        dst = att.at[:, pl.ds(pl.multiple_of(head * size, size), size)]
        if local:
            return pltpu.make_async_copy(src, dst, a_recv.at[head])
        return rdma(src, dst, a_send.at[j, dx, dc], a_recv.at[head], j * 2 + c, xx * 2 + cc)

    for j in range(depth):
        first = pl.multiple_of((2 * j + c) * span, span)
        length = (2 * j + 2) * span
        queries = jnp.dot(
            toks[pl.ds(first, span), :], wq[...], preferred_element_type=jnp.float32
        ).astype(jnp.bfloat16)
        logits = lax.dot_general(
            queries, keys[:length, :], (((1,), (1,)), ((), ())), preferred_element_type=jnp.float32
        )
        logits = logits * scale + cumc[pl.ds(first, span), :1] - cums[:1, :length]
        key_pos = lax.broadcasted_iota(jnp.int32, logits.shape, 1)
        query_pos = first + lax.broadcasted_iota(jnp.int32, logits.shape, 0)
        logits = jnp.where(key_pos <= query_pos, logits, -1e30)
        probs = jnp.exp(logits - jnp.max(logits, axis=1, keepdims=True))
        total = jnp.sum(probs, axis=1, keepdims=True)
        result = jnp.dot(
            probs.astype(jnp.bfloat16), vals[:length, :], preferred_element_type=jnp.float32
        )
        mine[pl.ds(j * span, span), :] = (result / total).astype(jnp.bfloat16)
        here = jnp.logical_and(home, z == j)
        for dx in range(2):
            for dc in range(2):
                if dx or dc:
                    deliver(j, dx, dc, False).start()

        @pl.when(here)
        def _():
            deliver(j, 0, 0, True).start()

        @pl.when(jnp.logical_not(here))
        def _():
            deliver(j, 0, 0, False).start()

        ow.corner(j)

    for j in range(depth):
        ow.partner(j)
    ow.keep.wait()
    for h in range(heads):
        ref = att.at[:, pl.ds(h * size, size)]
        pltpu.make_async_copy(ref, ref, a_recv.at[h]).wait()

    deep, wide = ow_ref.shape
    pieces = []
    for s in range(2 * depth):
        acc = None
        for t in range(4):
            term = jnp.dot(
                att[:, t * deep : (t + 1) * deep],
                outw[(s * 4 + t) * deep : (s * 4 + t + 1) * deep, :],
                preferred_element_type=jnp.float32,
            )
            acc = term if acc is None else acc + term
        pieces.append(acc)
    summed = jnp.concatenate(pieces, axis=1)
    normed = summed * lax.rsqrt(jnp.mean(summed * summed, axis=-1, keepdims=True) + 1e-06)
    out_ref[...] = (normed * gain_ref[...]).astype(jnp.bfloat16)

    for copy in tok.sent + ow.sent:
        copy.wait_send()
    for j in range(1, depth):
        for copy in send_w(j):
            copy.wait_send()

    @pl.when(jnp.logical_not(home))
    def _():
        for copy in send_w(0):
            copy.wait_send()

    @pl.when(home)
    def _():
        for copy in pass_w():
            copy.wait_send()

    for j in range(depth):
        for dx in range(2):
            for dc in range(2):
                if dx or dc:
                    deliver(j, dx, dc, False).wait_send()

        @pl.when(jnp.logical_not(jnp.logical_and(home, z == j)))
        def _():
            deliver(j, 0, 0, False).wait_send()


def head_per_chip(depth, tokens, qw, kw, vw, gw, fb, ow, gain):
    n_sp, n_tp = lax.axis_size("sp"), lax.axis_size("tp")
    n = n_sp * n_tp
    own, width = tokens.shape
    seq = own * n
    rows = qw.shape[0]
    size = qw.shape[1] // gw.shape[1]
    deep, wide = ow.shape
    gates = jnp.zeros((16, rows), jnp.bfloat16).at[: gw.shape[1]].set(gw.T)
    bias = jnp.zeros((8, 128), jnp.float32).at[: fb.shape[0]].set(fb[:, None])
    vm = pl.BlockSpec(memory_space=pltpu.VMEM)
    bf, f32 = jnp.bfloat16, jnp.float32
    dma = pltpu.SemaphoreType.DMA
    return pl.pallas_call(
        lambda *refs: layer(depth, size, *refs),
        out_shape=jax.ShapeDtypeStruct((own, wide * n_sp), bf),
        in_specs=[vm] * 8,
        out_specs=vm,
        scratch_shapes=[
            pltpu.VMEM((seq, width), bf),
            pltpu.VMEM((n * deep, wide), bf),
            pltpu.VMEM((rows * n_sp, size), bf),
            pltpu.VMEM((rows * n_sp, 2 * size), bf),
            pltpu.VMEM((16, rows * n_sp), bf),
            pltpu.VMEM((8, 128), f32),
            pltpu.VMEM((seq, size), bf),
            pltpu.VMEM((seq, size), bf),
            pltpu.VMEM((8, seq), f32),
            pltpu.VMEM((seq, 128), f32),
            pltpu.VMEM((seq // 2, size), bf),
            pltpu.VMEM((own, deep * n_tp), bf),
            dma((10, depth)),
            dma((10, depth)),
            dma((10, depth)),
            dma((10, depth)),
            dma((4, depth)),
            dma((4, depth, 2)),
            dma((4,)),
            dma((4,)),
            dma((depth, 2, 2)),
            dma((4 * depth,)),
            dma((3,)),
        ],
        compiler_params=pltpu.CompilerParams(has_side_effects=True, vmem_limit_bytes=60 * 2**20),
        name="layer",
    )(tokens, qw, kw, vw, gates, bias, ow, gain.reshape(1, -1))


def on_any(tokens, qw, kw, vw, gw, fb, ow, gain):
    n_sp, n_tp = lax.axis_size("sp"), lax.axis_size("tp")
    depth = n_sp // 2
    fits = n_sp % 2 == 0 and n_tp == 4 and gw.shape[1] == depth and depth <= 8
    tiles = qw.shape[1] == 128 * depth and qw.shape[0] == 128 and ow.shape[1] % 128 == 0
    if fits and tiles:
        return head_per_chip(depth, tokens, qw, kw, vw, gw, fb, ow, gain)
    return on_device(tokens, qw, kw, vw, gw, fb, ow, gain)


def solution(mesh):
    placed = (
        P(("sp", "tp"), None),
        P("sp", "tp"),
        P("sp", "tp"),
        P("sp", "tp"),
        P("sp", "tp"),
        P("tp"),
        P("tp", "sp"),
        P(),
    )
    return jax.shard_map(
        on_any, mesh=mesh, in_specs=placed, out_specs=P(("sp", "tp"), None), check_vma=False
    )
```

```python
import math

import jax
import jax.numpy as jnp
from jax import lax
from jax.experimental import pallas as pl
from jax.experimental.pallas import tpu as pltpu
from jax.sharding import PartitionSpec as P


def on_whole(shard, axis, dim, block):
    whole = lax.all_gather(shard, axis, axis=dim, tiled=True)
    return block(whole, jnp.int32(0))


def over_all(shard, axis, dim, absorb, state):
    everything = jax.tree.map(lambda a: lax.all_gather(a, axis, axis=dim, tiled=True), shard)
    return absorb(state, everything, jnp.int32(0))


def own_rows(product, width, axis):
    everything = product(jnp.int32(0), lax.axis_size(axis) * width)
    own = lax.psum_scatter(everything, axis, scatter_dimension=0, tiled=True)
    return own


def on_device(
    tokens, query_weight, key_weight, value_weight, gate_weight, forget_bias, out_weight, out_gain
):
    width = query_weight.shape[1]
    heads = gate_weight.shape[1]
    head_size = width // heads
    whole_q = lax.all_gather(query_weight, "sp", axis=0, tiled=True)
    whole_k = lax.all_gather(key_weight, "sp", axis=0, tiled=True)
    whole_v = lax.all_gather(value_weight, "sp", axis=0, tiled=True)
    whole_g = lax.all_gather(gate_weight, "sp", axis=0, tiled=True)
    joined = jnp.concatenate([whole_q, whole_k, whole_v, whole_g], axis=1)

    def project(piece, start):
        return jnp.dot(piece, joined, preferred_element_type=jnp.float32)

    projected = on_whole(tokens, "tp", 0, project)
    block = projected.shape[0]
    queries = projected[:, :width].astype(jnp.bfloat16).reshape(block, heads, head_size)
    keys = projected[:, width : 2 * width].astype(jnp.bfloat16).reshape(block, heads, head_size)
    values = (
        projected[:, 2 * width : 3 * width].astype(jnp.bfloat16).reshape(block, heads, head_size)
    )
    seq_len = block * lax.axis_size("sp")
    log_gate = jax.nn.log_sigmoid(projected[:, 3 * width :] + forget_bias + math.log(seq_len))
    gates_all = lax.all_gather(log_gate, "sp", axis=0, tiled=True)
    cumulative = jnp.cumsum(gates_all, axis=0)
    first = lax.axis_index("sp") * block
    query_cum = lax.dynamic_slice_in_dim(cumulative, first, block, 0)
    query_pos = first + jnp.arange(block, dtype=jnp.int32)
    scale = head_size ** (-0.5)

    def update(carry, piece, start):
        run_max, run_sum, run_acc = carry
        key_piece, value_piece = piece
        length = key_piece.shape[0]
        key_cum = lax.dynamic_slice_in_dim(cumulative, start, length, 0)
        logits = (
            jnp.einsum("qhd,khd->hqk", queries, key_piece, preferred_element_type=jnp.float32)
            * scale
        )
        logits = logits + query_cum.T[:, :, None] - key_cum.T[:, None, :]
        key_pos = start + jnp.arange(length, dtype=jnp.int32)
        allowed = (key_pos[None, :] <= query_pos[:, None])[None]
        logits = jnp.where(allowed, logits, -1e30)
        new_max = jnp.maximum(run_max, jnp.max(logits, axis=-1))
        probs = jnp.where(allowed, jnp.exp(logits - new_max[..., None]), 0.0)
        factor = jnp.exp(run_max - new_max)
        new_sum = run_sum * factor + jnp.sum(probs, axis=-1)
        new_acc = run_acc * factor[..., None] + jnp.einsum(
            "hqk,khd->hqd", probs, value_piece.astype(jnp.float32)
        )
        return (new_max, new_sum, new_acc)

    def attend(carry, piece, start):
        return lax.cond(
            start > first + block - 1,
            lambda state: state,
            lambda state: update(state, piece, start),
            carry,
        )

    initial = (
        jnp.full((heads, block), -1e30, jnp.float32),
        jnp.zeros((heads, block), jnp.float32),
        jnp.zeros((heads, block, head_size), jnp.float32),
    )
    run_max, run_sum, run_acc = over_all((keys, values), "sp", 0, attend, initial)
    attended = (
        (run_acc / run_sum[..., None]).transpose(1, 0, 2).reshape(block, width).astype(jnp.bfloat16)
    )
    out_full = lax.all_gather(out_weight, "sp", axis=1, tiled=True)
    rows = tokens.shape[0]

    def term(start, count):
        return jnp.dot(
            lax.dynamic_slice_in_dim(attended, start, count, 0),
            out_full,
            preferred_element_type=jnp.float32,
        )

    summed = own_rows(term, rows, "tp")
    normed = summed * lax.rsqrt(jnp.mean(summed * summed, axis=-1, keepdims=True) + 1e-06)
    return (normed * out_gain).astype(jnp.bfloat16)


MESH = pl.DeviceIdType.MESH
Z_, X_, Y_, DA, DB, PC, PX, PY, PA, PB = range(10)


def rdma(src, dst, send, recv, sp, tp):
    return pltpu.make_async_remote_copy(
        src_ref=src,
        dst_ref=dst,
        send_sem=send,
        recv_sem=recv,
        device_id={"sp": sp, "tp": tp},
        device_id_type=MESH,
    )


class Place:
    def __init__(self, depth):
        sp, tp = lax.axis_index("sp"), lax.axis_index("tp")
        self.depth, self.sp, self.tp = depth, sp, tp
        self.z, self.y = sp // 2, lax.rem(sp, 2)
        self.x, self.c = tp // 2, lax.rem(tp, 2)

    def back(self, j):
        return lax.rem(self.z + self.depth - j, self.depth)

    def ahead(self, j):
        return lax.rem(self.z + j, self.depth)


class Gather:
    def __init__(self, at, own, buf, send, recv, local):
        self.at, self.own, self.buf = at, own, buf
        self.send, self.recv, self.local = send, recv, local
        self.rows = own.shape[0]
        self.sent = []

    def block(self, z, y, x, c, half=None):
        start = (((z * 2 + y) * 2 + x) * 2 + c) * self.rows
        size = self.rows
        if half is not None:
            size = self.rows // 2
            start = start + half * size
        return self.buf.at[pl.ds(pl.multiple_of(start, size), size)]

    def go(self, kind, j, dst, sp, tp, src=None):
        copy = rdma(
            dst if src is None else src,
            dst,
            self.send.at[kind, j],
            self.recv.at[kind, j],
            sp,
            tp,
        )
        copy.start()
        self.sent.append(copy)

    def arrived(self, kind, j, ref):
        pltpu.make_async_copy(ref, ref, self.recv.at[kind, j]).wait()

    def to_x(self, kind, j, ref, src=None):
        a = self.at
        self.go(kind, j, ref, a.sp, (1 - a.x) * 2 + a.c, src)

    def to_y(self, kind, j, ref, src=None):
        a = self.at
        self.go(kind, j, ref, a.z * 2 + 1 - a.y, a.tp, src)

    def to_core(self, kind, j, ref, src=None):
        a = self.at
        self.go(kind, j, ref, a.sp, a.x * 2 + 1 - a.c, src)

    def begin(self):
        a = self.at
        mine = self.block(a.z, a.y, a.x, a.c)
        self.keep = pltpu.make_async_copy(self.own, mine, self.local)
        self.keep.start()
        self.to_x(X_, 0, mine, self.own)
        self.to_y(Y_, 0, mine, self.own)
        for j in range(1, a.depth):
            self.go(Z_, j, mine, a.ahead(j) * 2 + a.y, a.tp, self.own)
        self.to_core(PC, 0, mine, self.own)

    def column(self, j):
        a = self.at
        ref = self.block(a.back(j), a.y, a.x, a.c)
        self.arrived(Z_, j, ref)
        self.to_x(X_, j, ref)
        self.to_y(Y_, j, ref)
        self.to_core(PC, j, ref)

    def sides(self, j):
        a = self.at
        z = a.back(j)
        ref = self.block(z, a.y, 1 - a.x, a.c)
        self.arrived(X_, j, ref)
        self.to_y(DA, j, self.block(z, a.y, 1 - a.x, a.c, 0))
        self.to_core(PX, j, ref)
        ref = self.block(z, 1 - a.y, a.x, a.c)
        self.arrived(Y_, j, ref)
        self.to_x(DB, j, self.block(z, 1 - a.y, a.x, a.c, 1))
        self.to_core(PY, j, ref)

    def corner(self, j):
        a = self.at
        z = a.back(j)
        for kind, onward, half in ((DA, PA, 0), (DB, PB, 1)):
            ref = self.block(z, 1 - a.y, 1 - a.x, a.c, half)
            self.arrived(kind, j, ref)
            self.to_core(onward, j, ref)

    def partner(self, j):
        a = self.at
        z, c = a.back(j), 1 - a.c
        self.arrived(PC, j, self.block(z, a.y, a.x, c))
        self.arrived(PX, j, self.block(z, a.y, 1 - a.x, c))
        self.arrived(PY, j, self.block(z, 1 - a.y, a.x, c))
        self.arrived(PA, j, self.block(z, 1 - a.y, 1 - a.x, c, 0))
        self.arrived(PB, j, self.block(z, 1 - a.y, 1 - a.x, c, 1))

    def end(self):
        self.keep.wait()
        for copy in self.sent:
            copy.wait_send()


def layer(
    depth, size, tok_ref, q_ref, k_ref, v_ref, g_ref, b_ref, ow_ref, gain_ref, out_ref,
    toks, outw, wq, wkv, gates, bias, keys, vals, cums, cumc, mine, att,
    tok_send, tok_recv, ow_send, ow_recv, w_send, w_recv, p_send, p_recv, a_send, a_recv, keep,
):
    at = Place(depth)
    z, y, x, c = at.z, at.y, at.x, at.c
    home = y == c
    seq = toks.shape[0]
    heads = 4 * depth
    rows = q_ref.shape[0]
    tok = Gather(at, tok_ref, toks, tok_send, tok_recv, keep.at[0])
    ow = Gather(at, ow_ref, outw, ow_send, ow_recv, keep.at[1])

    def w_parts(head, row_block):
        cols = pl.ds(pl.multiple_of(head * size, size), size)
        place = pl.ds(pl.multiple_of(row_block * rows, rows), rows)
        return (
            (q_ref.at[:, cols], wq.at[place]),
            (k_ref.at[:, cols], wkv.at[place, pl.ds(0, size)]),
            (v_ref.at[:, cols], wkv.at[place, pl.ds(size, size)]),
            (g_ref, gates.at[:, place]),
        )

    away = jnp.where(home, 0, 1)

    def send_w(j):
        head = at.ahead(j)
        return [
            rdma(a, b, w_send.at[i, j], w_recv.at[i, j, away], head * 2 + c, at.tp)
            for i, (a, b) in enumerate(w_parts(head, at.sp))
        ]

    def keep_w():
        return [
            pltpu.make_async_copy(a, b, w_recv.at[i, 0, 0])
            for i, (a, b) in enumerate(w_parts(z, at.sp))
        ]

    def pass_w():
        whole = ((wq, wq), (wkv, wkv), (gates, gates), (b_ref, bias))
        return [
            rdma(a, b, p_send.at[i], p_recv.at[i], at.sp, x * 2 + 1 - c)
            for i, (a, b) in enumerate(whole)
        ]

    barrier = pltpu.get_barrier_semaphore()
    n_sp, n_tp = 2 * depth, 4
    for ds in range(n_sp):
        for dt in range(n_tp):
            if ds or dt:
                peer = {"sp": lax.rem(at.sp + ds, n_sp), "tp": lax.rem(at.tp + dt, n_tp)}
                pl.semaphore_signal(barrier, inc=1, device_id=peer, device_id_type=MESH)
    pl.semaphore_wait(barrier, n_sp * n_tp - 1)

    tok.begin()
    for j in range(1, depth):
        for copy in send_w(j):
            copy.start()

    @pl.when(home)
    def _():
        for copy in keep_w():
            copy.start()

    @pl.when(jnp.logical_not(home))
    def _():
        for copy in send_w(0):
            copy.start()

    tok.sides(0)
    for j in range(1, depth):
        tok.column(j)
    ow.begin()
    for j in range(1, depth):
        tok.sides(j)
    for j in range(depth):
        tok.corner(j)

    @pl.when(home)
    def _():
        for j in range(depth):
            for e in range(2):
                for i, (_a, b) in enumerate(w_parts(z, at.back(j) * 2 + (y if e == 0 else 1 - y))):
                    pltpu.make_async_copy(b, b, w_recv.at[i, j, e]).wait()
        for copy in pass_w():
            copy.start()
        moved = pltpu.make_async_copy(b_ref, bias, keep.at[2])
        moved.start()
        moved.wait()

    tok.keep.wait()
    for j in range(depth):
        tok.partner(j)
    ow.sides(0)
    for j in range(1, depth):
        ow.column(j)

    @pl.when(jnp.logical_not(home))
    def _():
        for i, ref in enumerate((wq, wkv, gates, bias)):
            pltpu.make_async_copy(ref, ref, p_recv.at[i]).wait()

    raw = lax.dot_general(
        gates[...], toks[...], (((1,), (1,)), ((), ())), preferred_element_type=jnp.float32
    )[:8]
    raw = raw + bias[:, :1] + math.log(seq)
    run = jnp.minimum(raw, 0.0) - jnp.log1p(jnp.exp(-jnp.abs(raw)))
    lane = lax.broadcasted_iota(jnp.int32, run.shape, 1)
    step = 1
    while step < seq:
        run = run + jnp.where(lane >= step, pltpu.roll(run, step, 1), 0.0)
        step *= 2
    which = lax.broadcasted_iota(jnp.int32, run.shape, 0)
    chosen = jnp.sum(jnp.where(which == z, run, 0.0), axis=0, keepdims=True)
    cums[...] = jnp.broadcast_to(chosen, cums.shape)
    cumc[...] = jnp.broadcast_to(chosen, (128, seq)).T

    span = seq // (2 * depth)
    for i in range(2 * depth):
        part = pl.ds(i * span, span)
        both = jnp.dot(toks[part, :], wkv[...], preferred_element_type=jnp.float32)
        keys[part, :] = both[:, :size].astype(jnp.bfloat16)
        vals[part, :] = both[:, size:].astype(jnp.bfloat16)
    for j in range(1, depth):
        ow.sides(j)

    scale = size ** (-0.5)
    own = span // 4
    head = (2 * x + y) * depth + z

    def deliver(j, dx, dc, local):
        xx = x if dx == 0 else 1 - x
        cc = c if dc == 0 else 1 - c
        start = pl.multiple_of(j * span + (xx * 2 + cc) * own, own)
        src = mine.at[pl.ds(start, own)]
        dst = att.at[:, pl.ds(pl.multiple_of(head * size, size), size)]
        if local:
            return pltpu.make_async_copy(src, dst, a_recv.at[head])
        return rdma(src, dst, a_send.at[j, dx, dc], a_recv.at[head], j * 2 + c, xx * 2 + cc)

    for j in range(depth):
        first = pl.multiple_of((2 * j + c) * span, span)
        length = (2 * j + 2) * span
        queries = jnp.dot(
            toks[pl.ds(first, span), :], wq[...], preferred_element_type=jnp.float32
        ).astype(jnp.bfloat16)
        logits = lax.dot_general(
            queries, keys[:length, :], (((1,), (1,)), ((), ())), preferred_element_type=jnp.float32
        )
        logits = logits * scale + cumc[pl.ds(first, span), :1] - cums[:1, :length]
        key_pos = lax.broadcasted_iota(jnp.int32, logits.shape, 1)
        query_pos = first + lax.broadcasted_iota(jnp.int32, logits.shape, 0)
        logits = jnp.where(key_pos <= query_pos, logits, -1e30)
        probs = jnp.exp(logits - jnp.max(logits, axis=1, keepdims=True))
        total = jnp.sum(probs, axis=1, keepdims=True)
        result = jnp.dot(
            probs.astype(jnp.bfloat16), vals[:length, :], preferred_element_type=jnp.float32
        )
        mine[pl.ds(j * span, span), :] = (result / total).astype(jnp.bfloat16)
        here = jnp.logical_and(home, z == j)
        for dx in range(2):
            for dc in range(2):
                if dx or dc:
                    deliver(j, dx, dc, False).start()

        @pl.when(here)
        def _():
            deliver(j, 0, 0, True).start()

        @pl.when(jnp.logical_not(here))
        def _():
            deliver(j, 0, 0, False).start()

        ow.corner(j)

    for j in range(depth):
        ow.partner(j)
    ow.keep.wait()
    for h in range(heads):
        ref = att.at[:, pl.ds(h * size, size)]
        pltpu.make_async_copy(ref, ref, a_recv.at[h]).wait()

    deep, wide = ow_ref.shape
    pieces = []
    for s in range(2 * depth):
        acc = None
        for t in range(4):
            term = jnp.dot(
                att[:, t * deep : (t + 1) * deep],
                outw[(s * 4 + t) * deep : (s * 4 + t + 1) * deep, :],
                preferred_element_type=jnp.float32,
            )
            acc = term if acc is None else acc + term
        pieces.append(acc)
    summed = jnp.concatenate(pieces, axis=1)
    normed = summed * lax.rsqrt(jnp.mean(summed * summed, axis=-1, keepdims=True) + 1e-06)
    out_ref[...] = (normed * gain_ref[...]).astype(jnp.bfloat16)

    for copy in tok.sent + ow.sent:
        copy.wait_send()
    for j in range(1, depth):
        for copy in send_w(j):
            copy.wait_send()

    @pl.when(jnp.logical_not(home))
    def _():
        for copy in send_w(0):
            copy.wait_send()

    @pl.when(home)
    def _():
        for copy in pass_w():
            copy.wait_send()

    for j in range(depth):
        for dx in range(2):
            for dc in range(2):
                if dx or dc:
                    deliver(j, dx, dc, False).wait_send()

        @pl.when(jnp.logical_not(jnp.logical_and(home, z == j)))
        def _():
            deliver(j, 0, 0, False).wait_send()


def head_per_chip(depth, tokens, qw, kw, vw, gw, fb, ow, gain):
    n_sp, n_tp = lax.axis_size("sp"), lax.axis_size("tp")
    n = n_sp * n_tp
    own, width = tokens.shape
    seq = own * n
    rows = qw.shape[0]
    size = qw.shape[1] // gw.shape[1]
    deep, wide = ow.shape
    gates = jnp.zeros((16, rows), jnp.bfloat16).at[: gw.shape[1]].set(gw.T)
    bias = jnp.zeros((8, 128), jnp.float32).at[: fb.shape[0]].set(fb[:, None])
    vm = pl.BlockSpec(memory_space=pltpu.VMEM)
    bf, f32 = jnp.bfloat16, jnp.float32
    dma = pltpu.SemaphoreType.DMA
    return pl.pallas_call(
        lambda *refs: layer(depth, size, *refs),
        out_shape=jax.ShapeDtypeStruct((own, wide * n_sp), bf),
        in_specs=[vm] * 8,
        out_specs=vm,
        scratch_shapes=[
            pltpu.VMEM((seq, width), bf),
            pltpu.VMEM((n * deep, wide), bf),
            pltpu.VMEM((rows * n_sp, size), bf),
            pltpu.VMEM((rows * n_sp, 2 * size), bf),
            pltpu.VMEM((16, rows * n_sp), bf),
            pltpu.VMEM((8, 128), f32),
            pltpu.VMEM((seq, size), bf),
            pltpu.VMEM((seq, size), bf),
            pltpu.VMEM((8, seq), f32),
            pltpu.VMEM((seq, 128), f32),
            pltpu.VMEM((seq // 2, size), bf),
            pltpu.VMEM((own, deep * n_tp), bf),
            dma((10, depth)),
            dma((10, depth)),
            dma((10, depth)),
            dma((10, depth)),
            dma((4, depth)),
            dma((4, depth, 2)),
            dma((4,)),
            dma((4,)),
            dma((depth, 2, 2)),
            dma((4 * depth,)),
            dma((3,)),
        ],
        compiler_params=pltpu.CompilerParams(
            collective_id=0, has_side_effects=True, vmem_limit_bytes=60 * 2**20
        ),
        name="layer",
    )(tokens, qw, kw, vw, gates, bias, ow, gain.reshape(1, -1))


def on_any(tokens, qw, kw, vw, gw, fb, ow, gain):
    n_sp, n_tp = lax.axis_size("sp"), lax.axis_size("tp")
    depth = n_sp // 2
    fits = n_sp % 2 == 0 and n_tp == 4 and gw.shape[1] == depth and depth <= 8
    tiles = qw.shape[1] == 128 * depth and qw.shape[0] == 128 and ow.shape[1] % 128 == 0
    if fits and tiles:
        return head_per_chip(depth, tokens, qw, kw, vw, gw, fb, ow, gain)
    return on_device(tokens, qw, kw, vw, gw, fb, ow, gain)


def solution(mesh):
    placed = (
        P(("sp", "tp"), None),
        P("sp", "tp"),
        P("sp", "tp"),
        P("sp", "tp"),
        P("sp", "tp"),
        P("tp"),
        P("tp", "sp"),
        P(),
    )
    return jax.shard_map(
        on_any, mesh=mesh, in_specs=placed, out_specs=P(("sp", "tp"), None), check_vma=False
    )
```

```python
import math

import jax
import jax.numpy as jnp
from jax import lax
from jax.experimental import pallas as pl
from jax.experimental.pallas import tpu as pltpu
from jax.sharding import PartitionSpec as P


def on_whole(shard, axis, dim, block):
    whole = lax.all_gather(shard, axis, axis=dim, tiled=True)
    return block(whole, jnp.int32(0))


def over_all(shard, axis, dim, absorb, state):
    everything = jax.tree.map(lambda a: lax.all_gather(a, axis, axis=dim, tiled=True), shard)
    return absorb(state, everything, jnp.int32(0))


def own_rows(product, width, axis):
    everything = product(jnp.int32(0), lax.axis_size(axis) * width)
    own = lax.psum_scatter(everything, axis, scatter_dimension=0, tiled=True)
    return own


def on_device(
    tokens, query_weight, key_weight, value_weight, gate_weight, forget_bias, out_weight, out_gain
):
    width = query_weight.shape[1]
    heads = gate_weight.shape[1]
    head_size = width // heads
    whole_q = lax.all_gather(query_weight, "sp", axis=0, tiled=True)
    whole_k = lax.all_gather(key_weight, "sp", axis=0, tiled=True)
    whole_v = lax.all_gather(value_weight, "sp", axis=0, tiled=True)
    whole_g = lax.all_gather(gate_weight, "sp", axis=0, tiled=True)
    joined = jnp.concatenate([whole_q, whole_k, whole_v, whole_g], axis=1)

    def project(piece, start):
        return jnp.dot(piece, joined, preferred_element_type=jnp.float32)

    projected = on_whole(tokens, "tp", 0, project)
    block = projected.shape[0]
    queries = projected[:, :width].astype(jnp.bfloat16).reshape(block, heads, head_size)
    keys = projected[:, width : 2 * width].astype(jnp.bfloat16).reshape(block, heads, head_size)
    values = (
        projected[:, 2 * width : 3 * width].astype(jnp.bfloat16).reshape(block, heads, head_size)
    )
    seq_len = block * lax.axis_size("sp")
    log_gate = jax.nn.log_sigmoid(projected[:, 3 * width :] + forget_bias + math.log(seq_len))
    gates_all = lax.all_gather(log_gate, "sp", axis=0, tiled=True)
    cumulative = jnp.cumsum(gates_all, axis=0)
    first = lax.axis_index("sp") * block
    query_cum = lax.dynamic_slice_in_dim(cumulative, first, block, 0)
    query_pos = first + jnp.arange(block, dtype=jnp.int32)
    scale = head_size ** (-0.5)

    def update(carry, piece, start):
        run_max, run_sum, run_acc = carry
        key_piece, value_piece = piece
        length = key_piece.shape[0]
        key_cum = lax.dynamic_slice_in_dim(cumulative, start, length, 0)
        logits = (
            jnp.einsum("qhd,khd->hqk", queries, key_piece, preferred_element_type=jnp.float32)
            * scale
        )
        logits = logits + query_cum.T[:, :, None] - key_cum.T[:, None, :]
        key_pos = start + jnp.arange(length, dtype=jnp.int32)
        allowed = (key_pos[None, :] <= query_pos[:, None])[None]
        logits = jnp.where(allowed, logits, -1e30)
        new_max = jnp.maximum(run_max, jnp.max(logits, axis=-1))
        probs = jnp.where(allowed, jnp.exp(logits - new_max[..., None]), 0.0)
        factor = jnp.exp(run_max - new_max)
        new_sum = run_sum * factor + jnp.sum(probs, axis=-1)
        new_acc = run_acc * factor[..., None] + jnp.einsum(
            "hqk,khd->hqd", probs, value_piece.astype(jnp.float32)
        )
        return (new_max, new_sum, new_acc)

    def attend(carry, piece, start):
        return lax.cond(
            start > first + block - 1,
            lambda state: state,
            lambda state: update(state, piece, start),
            carry,
        )

    initial = (
        jnp.full((heads, block), -1e30, jnp.float32),
        jnp.zeros((heads, block), jnp.float32),
        jnp.zeros((heads, block, head_size), jnp.float32),
    )
    run_max, run_sum, run_acc = over_all((keys, values), "sp", 0, attend, initial)
    attended = (
        (run_acc / run_sum[..., None]).transpose(1, 0, 2).reshape(block, width).astype(jnp.bfloat16)
    )
    out_full = lax.all_gather(out_weight, "sp", axis=1, tiled=True)
    rows = tokens.shape[0]

    def term(start, count):
        return jnp.dot(
            lax.dynamic_slice_in_dim(attended, start, count, 0),
            out_full,
            preferred_element_type=jnp.float32,
        )

    summed = own_rows(term, rows, "tp")
    normed = summed * lax.rsqrt(jnp.mean(summed * summed, axis=-1, keepdims=True) + 1e-06)
    return (normed * out_gain).astype(jnp.bfloat16)


MESH = pl.DeviceIdType.MESH
Z_, X_, Y_, DA, DB, PC, PX, PY, PA, PB, ZD = range(11)


def rdma(src, dst, send, recv, sp, tp):
    return pltpu.make_async_remote_copy(
        src_ref=src,
        dst_ref=dst,
        send_sem=send,
        recv_sem=recv,
        device_id={"sp": sp, "tp": tp},
        device_id_type=MESH,
    )


class Place:
    def __init__(self, depth):
        sp, tp = lax.axis_index("sp"), lax.axis_index("tp")
        self.depth, self.sp, self.tp = depth, sp, tp
        self.z, self.y = sp // 2, lax.rem(sp, 2)
        self.x, self.c = tp // 2, lax.rem(tp, 2)

    def back(self, j):
        return lax.rem(self.z + self.depth - j, self.depth)

    def ahead(self, j):
        return lax.rem(self.z + j, self.depth)

    def nearest(self, k):
        pick = 0
        for z in range(self.depth):
            others = sorted((abs(o - z), (z - o) % self.depth) for o in range(self.depth))
            pick = pick + jnp.where(self.z == z, others[k][1], 0)
        return pick


class Gather:
    def __init__(self, at, own, buf, send, recv, local, parts):
        self.at, self.own, self.buf = at, own, buf
        self.send, self.recv, self.local = send, recv, local
        self.rows = own.shape[0]
        self.cut = self.rows // parts
        self.sent = []
        self.maybe = []

    def block(self, z, y, x, c, half=None):
        start = (((z * 2 + y) * 2 + x) * 2 + c) * self.rows
        size = self.rows
        if half is not None:
            size = self.rows - self.cut if half else self.cut
            start = start + half * self.cut
        return self.buf.at[pl.ds(pl.multiple_of(start, self.cut), size)]

    def go(self, kind, j, dst, sp, tp, src=None):
        copy = rdma(
            dst if src is None else src,
            dst,
            self.send.at[kind, j],
            self.recv.at[kind, j],
            sp,
            tp,
        )
        copy.start()
        self.sent.append(copy)

    def arrived(self, kind, j, ref):
        pltpu.make_async_copy(ref, ref, self.recv.at[kind, j]).wait()

    def to_x(self, kind, j, ref, src=None):
        a = self.at
        self.go(kind, j, ref, a.sp, (1 - a.x) * 2 + a.c, src)

    def to_y(self, kind, j, ref, src=None):
        a = self.at
        self.go(kind, j, ref, a.z * 2 + 1 - a.y, a.tp, src)

    def to_core(self, kind, j, ref, src=None):
        a = self.at
        self.go(kind, j, ref, a.sp, a.x * 2 + 1 - a.c, src)

    def begin(self):
        a = self.at
        mine = self.block(a.z, a.y, a.x, a.c)
        self.keep = pltpu.make_async_copy(self.own, mine, self.local)
        self.keep.start()
        self.to_x(X_, 0, mine, self.own)
        self.to_y(Y_, 0, mine, self.own)
        self.along(a.z < a.depth - 1, Z_, 0, mine, a.ahead(1), 1, self.own)
        self.along(a.z > 0, ZD, 0, mine, a.back(1), a.depth - 1, self.own)
        self.to_core(PC, 0, mine, self.own)

    def along(self, when, kind, j, ref, z, k, src=None):
        a = self.at
        copy = rdma(
            ref if src is None else src,
            ref,
            self.send.at[kind, j],
            self.recv.at[Z_, k],
            z * 2 + a.y,
            a.tp,
        )
        self.maybe.append((when, copy))

        @pl.when(when)
        def _():
            copy.start()

    def column(self, j):
        a = self.at
        ref = self.block(a.back(j), a.y, a.x, a.c)
        self.arrived(Z_, j, ref)
        below = j <= a.z
        up = jnp.logical_and(below, a.z < a.depth - 1)
        down = jnp.logical_and(jnp.logical_not(below), a.z > 0)
        self.along(up, Z_, j, ref, a.ahead(1), lax.rem(j + 1, a.depth))
        self.along(down, ZD, j, ref, a.back(1), j - 1)
        self.to_x(X_, j, ref)
        self.to_y(Y_, j, ref)
        self.to_core(PC, j, ref)

    def sides(self, j):
        a = self.at
        z = a.back(j)
        ref = self.block(z, a.y, 1 - a.x, a.c)
        self.arrived(X_, j, ref)
        self.to_y(DA, j, self.block(z, a.y, 1 - a.x, a.c, 0))
        self.to_core(PX, j, ref)
        ref = self.block(z, 1 - a.y, a.x, a.c)
        self.arrived(Y_, j, ref)
        self.to_x(DB, j, self.block(z, 1 - a.y, a.x, a.c, 1))
        self.to_core(PY, j, ref)

    def corner(self, j):
        a = self.at
        z = a.back(j)
        for kind, onward, half in ((DA, PA, 0), (DB, PB, 1)):
            ref = self.block(z, 1 - a.y, 1 - a.x, a.c, half)
            self.arrived(kind, j, ref)
            self.to_core(onward, j, ref)

    def partner(self, j):
        a = self.at
        z, c = a.back(j), 1 - a.c
        self.arrived(PC, j, self.block(z, a.y, a.x, c))
        self.arrived(PX, j, self.block(z, a.y, 1 - a.x, c))
        self.arrived(PY, j, self.block(z, 1 - a.y, a.x, c))
        self.arrived(PA, j, self.block(z, 1 - a.y, 1 - a.x, c, 0))
        self.arrived(PB, j, self.block(z, 1 - a.y, 1 - a.x, c, 1))

    def end(self):
        for copy in self.sent:
            copy.wait_send()
        for when, copy in self.maybe:

            @pl.when(when)
            def _(copy=copy):
                copy.wait_send()


def layer(
    depth, size, tok_ref, q_ref, k_ref, v_ref, g_ref, b_ref, ow_ref, gain_ref, out_ref,
    toks, outw, wq, wkv, gates, bias, keys, vals, cums, cumc, mine, att,
    tok_send, tok_recv, ow_send, ow_recv, w_send, w_recv, p_send, p_recv, a_send, a_recv, keep,
):
    at = Place(depth)
    z, y, x, c = at.z, at.y, at.x, at.c
    home = y == c
    seq = toks.shape[0]
    heads = 4 * depth
    rows = q_ref.shape[0]
    tok = Gather(at, tok_ref, toks, tok_send, tok_recv, keep.at[0], 4)
    ow = Gather(at, ow_ref, outw, ow_send, ow_recv, keep.at[1], 2)

    def w_parts(head, row_block):
        cols = pl.ds(pl.multiple_of(head * size, size), size)
        place = pl.ds(pl.multiple_of(row_block * rows, rows), rows)
        return (
            (q_ref.at[:, cols], wq.at[place]),
            (k_ref.at[:, cols], wkv.at[place, pl.ds(0, size)]),
            (v_ref.at[:, cols], wkv.at[place, pl.ds(size, size)]),
            (g_ref, gates.at[:, place]),
        )

    away = jnp.where(home, 0, 1)

    def send_w(j):
        head = at.ahead(j)
        return [
            rdma(a, b, w_send.at[i, j], w_recv.at[i, j, away], head * 2 + c, at.tp)
            for i, (a, b) in enumerate(w_parts(head, at.sp))
        ]

    def keep_w():
        return [
            pltpu.make_async_copy(a, b, w_recv.at[i, 0, 0])
            for i, (a, b) in enumerate(w_parts(z, at.sp))
        ]

    def pass_w():
        whole = ((wq, wq), (wkv, wkv), (gates, gates), (b_ref, bias))
        return [
            rdma(a, b, p_send.at[i], p_recv.at[i], at.sp, x * 2 + 1 - c)
            for i, (a, b) in enumerate(whole)
        ]

    barrier = pltpu.get_barrier_semaphore()
    near = [(at.sp, x * 2 + 1 - c), (at.sp, (1 - x) * 2 + c), (z * 2 + 1 - y, at.tp)]

    def greet(sp, tp):
        peer = {"sp": sp, "tp": tp}
        pl.semaphore_signal(barrier, inc=1, device_id=peer, device_id_type=MESH)

    for sp, tp in near:
        greet(sp, tp)
    pl.when(z > 0)(lambda: greet(at.sp - 2, at.tp))
    pl.when(z < depth - 1)(lambda: greet(at.sp + 2, at.tp))
    ends = jnp.where(z > 0, 1, 0) + jnp.where(z < depth - 1, 1, 0)
    pl.semaphore_wait(barrier, len(near) + ends)

    tok.begin()

    @pl.when(home)
    def _():
        for copy in keep_w():
            copy.start()

    @pl.when(jnp.logical_not(home))
    def _():
        for copy in send_w(0):
            copy.start()

    def later_w(when, j):
        @pl.when(when)
        def _():
            for copy in send_w(depth - j):
                copy.start()

    order = [0] + [at.nearest(k) for k in range(1, depth)]
    for last, j in zip(order[:-1], order[1:]):
        tok.column(j)
        later_w(home, j)
        tok.sides(last)
        if last is not order[0]:
            later_w(jnp.logical_not(home), last)
    tok.sides(order[-1])
    later_w(jnp.logical_not(home), order[-1])
    ow.begin()
    tok.corner(order[0])

    @pl.when(home)
    def _():
        for j in range(depth):
            for e in range(2):
                for i, (_a, b) in enumerate(w_parts(z, at.back(j) * 2 + (y if e == 0 else 1 - y))):
                    pltpu.make_async_copy(b, b, w_recv.at[i, j, e]).wait()
        for copy in pass_w():
            copy.start()
        moved = pltpu.make_async_copy(b_ref, bias, keep.at[2])
        moved.start()
        moved.wait()

    for last, j in zip(order[:-1], order[1:]):
        tok.corner(j)
        ow.column(j)
        ow.sides(last)
    tok.keep.wait()
    for j in order:
        tok.partner(j)

    @pl.when(jnp.logical_not(home))
    def _():
        for i, ref in enumerate((wq, wkv, gates, bias)):
            pltpu.make_async_copy(ref, ref, p_recv.at[i]).wait()

    raw = lax.dot_general(
        gates[...], toks[...], (((1,), (1,)), ((), ())), preferred_element_type=jnp.float32
    )[:8]
    raw = raw + bias[:, :1] + math.log(seq)
    run = jnp.minimum(raw, 0.0) - jnp.log1p(jnp.exp(-jnp.abs(raw)))
    lane = lax.broadcasted_iota(jnp.int32, run.shape, 1)
    step = 1
    while step < seq:
        run = run + jnp.where(lane >= step, pltpu.roll(run, step, 1), 0.0)
        step *= 2
    which = lax.broadcasted_iota(jnp.int32, run.shape, 0)
    chosen = jnp.sum(jnp.where(which == z, run, 0.0), axis=0, keepdims=True)
    cums[...] = jnp.broadcast_to(chosen, cums.shape)
    cumc[...] = jnp.broadcast_to(chosen, (128, seq)).T

    span = seq // (2 * depth)
    for i in range(2 * depth):
        part = pl.ds(i * span, span)
        both = jnp.dot(toks[part, :], wkv[...], preferred_element_type=jnp.float32)
        keys[part, :] = both[:, :size].astype(jnp.bfloat16)
        vals[part, :] = both[:, size:].astype(jnp.bfloat16)
    ow.sides(order[-1])

    scale = size ** (-0.5)
    own = span // 4
    head = (2 * x + y) * depth + z

    def deliver(j, dx, dc, local):
        xx = x if dx == 0 else 1 - x
        cc = c if dc == 0 else 1 - c
        start = pl.multiple_of(j * span + (xx * 2 + cc) * own, own)
        src = mine.at[pl.ds(start, own)]
        dst = att.at[:, pl.ds(pl.multiple_of(head * size, size), size)]
        if local:
            return pltpu.make_async_copy(src, dst, a_recv.at[head])
        return rdma(src, dst, a_send.at[j, dx, dc], a_recv.at[head], j * 2 + c, xx * 2 + cc)

    for j in range(depth):
        first = pl.multiple_of((2 * j + c) * span, span)
        length = (2 * j + 2) * span
        queries = jnp.dot(
            toks[pl.ds(first, span), :], wq[...], preferred_element_type=jnp.float32
        ).astype(jnp.bfloat16)
        logits = lax.dot_general(
            queries, keys[:length, :], (((1,), (1,)), ((), ())), preferred_element_type=jnp.float32
        )
        logits = logits * scale + cumc[pl.ds(first, span), :1] - cums[:1, :length]
        key_pos = lax.broadcasted_iota(jnp.int32, logits.shape, 1)
        query_pos = first + lax.broadcasted_iota(jnp.int32, logits.shape, 0)
        logits = jnp.where(key_pos <= query_pos, logits, -1e30)
        probs = jnp.exp(logits - jnp.max(logits, axis=1, keepdims=True))
        total = jnp.sum(probs, axis=1, keepdims=True)
        result = jnp.dot(
            probs.astype(jnp.bfloat16), vals[:length, :], preferred_element_type=jnp.float32
        )
        mine[pl.ds(j * span, span), :] = (result / total).astype(jnp.bfloat16)
        here = jnp.logical_and(home, z == j)
        for dx in range(2):
            for dc in range(2):
                if dx or dc:
                    deliver(j, dx, dc, False).start()

        @pl.when(here)
        def _():
            deliver(j, 0, 0, True).start()

        @pl.when(jnp.logical_not(here))
        def _():
            deliver(j, 0, 0, False).start()

        ow.corner(order[j])

    for j in order:
        ow.partner(j)
    ow.keep.wait()
    for h in range(heads):
        ref = att.at[:, pl.ds(h * size, size)]
        pltpu.make_async_copy(ref, ref, a_recv.at[h]).wait()

    deep, wide = ow_ref.shape
    pieces = []
    for s in range(2 * depth):
        acc = None
        for t in range(4):
            term = jnp.dot(
                att[:, t * deep : (t + 1) * deep],
                outw[(s * 4 + t) * deep : (s * 4 + t + 1) * deep, :],
                preferred_element_type=jnp.float32,
            )
            acc = term if acc is None else acc + term
        pieces.append(acc)
    summed = jnp.concatenate(pieces, axis=1)
    normed = summed * lax.rsqrt(jnp.mean(summed * summed, axis=-1, keepdims=True) + 1e-06)
    out_ref[...] = (normed * gain_ref[...]).astype(jnp.bfloat16)

    tok.end()
    ow.end()
    for j in range(1, depth):
        for copy in send_w(j):
            copy.wait_send()

    @pl.when(jnp.logical_not(home))
    def _():
        for copy in send_w(0):
            copy.wait_send()

    @pl.when(home)
    def _():
        for copy in pass_w():
            copy.wait_send()

    for j in range(depth):
        for dx in range(2):
            for dc in range(2):
                if dx or dc:
                    deliver(j, dx, dc, False).wait_send()

        @pl.when(jnp.logical_not(jnp.logical_and(home, z == j)))
        def _():
            deliver(j, 0, 0, False).wait_send()


def head_per_chip(depth, tokens, qw, kw, vw, gw, fb, ow, gain):
    n_sp, n_tp = lax.axis_size("sp"), lax.axis_size("tp")
    n = n_sp * n_tp
    own, width = tokens.shape
    seq = own * n
    rows = qw.shape[0]
    size = qw.shape[1] // gw.shape[1]
    deep, wide = ow.shape
    gates = jnp.pad(gw.T, ((0, 16 - gw.shape[1]), (0, 0)))
    spread = jnp.broadcast_to(fb[:, None], (fb.shape[0], 128))
    bias = jnp.pad(spread, ((0, 8 - fb.shape[0]), (0, 0)))
    vm = pl.BlockSpec(memory_space=pltpu.VMEM)
    bf, f32 = jnp.bfloat16, jnp.float32
    dma = pltpu.SemaphoreType.DMA
    return pl.pallas_call(
        lambda *refs: layer(depth, size, *refs),
        out_shape=jax.ShapeDtypeStruct((own, wide * n_sp), bf),
        in_specs=[vm] * 8,
        out_specs=vm,
        scratch_shapes=[
            pltpu.VMEM((seq, width), bf),
            pltpu.VMEM((n * deep, wide), bf),
            pltpu.VMEM((rows * n_sp, size), bf),
            pltpu.VMEM((rows * n_sp, 2 * size), bf),
            pltpu.VMEM((16, rows * n_sp), bf),
            pltpu.VMEM((8, 128), f32),
            pltpu.VMEM((seq, size), bf),
            pltpu.VMEM((seq, size), bf),
            pltpu.VMEM((8, seq), f32),
            pltpu.VMEM((seq, 128), f32),
            pltpu.VMEM((seq // 2, size), bf),
            pltpu.VMEM((own, deep * n_tp), bf),
            dma((11, depth)),
            dma((11, depth)),
            dma((11, depth)),
            dma((11, depth)),
            dma((4, depth)),
            dma((4, depth, 2)),
            dma((4,)),
            dma((4,)),
            dma((depth, 2, 2)),
            dma((4 * depth,)),
            dma((3,)),
        ],
        compiler_params=pltpu.CompilerParams(
            collective_id=0, has_side_effects=True, vmem_limit_bytes=60 * 2**20
        ),
        name="layer",
    )(tokens, qw, kw, vw, gates, bias, ow, gain.reshape(1, -1))


def on_any(tokens, qw, kw, vw, gw, fb, ow, gain):
    n_sp, n_tp = lax.axis_size("sp"), lax.axis_size("tp")
    depth = n_sp // 2
    fits = n_sp % 2 == 0 and n_tp == 4 and gw.shape[1] == depth and depth <= 8
    tiles = qw.shape[1] == 128 * depth and qw.shape[0] == 128 and ow.shape[1] % 128 == 0
    if fits and tiles:
        return head_per_chip(depth, tokens, qw, kw, vw, gw, fb, ow, gain)
    return on_device(tokens, qw, kw, vw, gw, fb, ow, gain)


def solution(mesh):
    placed = (
        P(("sp", "tp"), None),
        P("sp", "tp"),
        P("sp", "tp"),
        P("sp", "tp"),
        P("sp", "tp"),
        P("tp"),
        P("tp", "sp"),
        P(),
    )
    return jax.shard_map(
        on_any, mesh=mesh, in_specs=placed, out_specs=P(("sp", "tp"), None), check_vma=False
    )
```

```python
import math

import jax
import jax.numpy as jnp
from jax import lax
from jax.experimental import pallas as pl
from jax.experimental.pallas import tpu as pltpu
from jax.sharding import PartitionSpec as P


def on_whole(shard, axis, dim, block):
    whole = lax.all_gather(shard, axis, axis=dim, tiled=True)
    return block(whole, jnp.int32(0))


def over_all(shard, axis, dim, absorb, state):
    everything = jax.tree.map(lambda a: lax.all_gather(a, axis, axis=dim, tiled=True), shard)
    return absorb(state, everything, jnp.int32(0))


def own_rows(product, width, axis):
    everything = product(jnp.int32(0), lax.axis_size(axis) * width)
    own = lax.psum_scatter(everything, axis, scatter_dimension=0, tiled=True)
    return own


def on_device(
    tokens, query_weight, key_weight, value_weight, gate_weight, forget_bias, out_weight, out_gain
):
    width = query_weight.shape[1]
    heads = gate_weight.shape[1]
    head_size = width // heads
    whole_q = lax.all_gather(query_weight, "sp", axis=0, tiled=True)
    whole_k = lax.all_gather(key_weight, "sp", axis=0, tiled=True)
    whole_v = lax.all_gather(value_weight, "sp", axis=0, tiled=True)
    whole_g = lax.all_gather(gate_weight, "sp", axis=0, tiled=True)
    joined = jnp.concatenate([whole_q, whole_k, whole_v, whole_g], axis=1)

    def project(piece, start):
        return jnp.dot(piece, joined, preferred_element_type=jnp.float32)

    projected = on_whole(tokens, "tp", 0, project)
    block = projected.shape[0]
    queries = projected[:, :width].astype(jnp.bfloat16).reshape(block, heads, head_size)
    keys = projected[:, width : 2 * width].astype(jnp.bfloat16).reshape(block, heads, head_size)
    values = (
        projected[:, 2 * width : 3 * width].astype(jnp.bfloat16).reshape(block, heads, head_size)
    )
    seq_len = block * lax.axis_size("sp")
    log_gate = jax.nn.log_sigmoid(projected[:, 3 * width :] + forget_bias + math.log(seq_len))
    gates_all = lax.all_gather(log_gate, "sp", axis=0, tiled=True)
    cumulative = jnp.cumsum(gates_all, axis=0)
    first = lax.axis_index("sp") * block
    query_cum = lax.dynamic_slice_in_dim(cumulative, first, block, 0)
    query_pos = first + jnp.arange(block, dtype=jnp.int32)
    scale = head_size ** (-0.5)

    def update(carry, piece, start):
        run_max, run_sum, run_acc = carry
        key_piece, value_piece = piece
        length = key_piece.shape[0]
        key_cum = lax.dynamic_slice_in_dim(cumulative, start, length, 0)
        logits = (
            jnp.einsum("qhd,khd->hqk", queries, key_piece, preferred_element_type=jnp.float32)
            * scale
        )
        logits = logits + query_cum.T[:, :, None] - key_cum.T[:, None, :]
        key_pos = start + jnp.arange(length, dtype=jnp.int32)
        allowed = (key_pos[None, :] <= query_pos[:, None])[None]
        logits = jnp.where(allowed, logits, -1e30)
        new_max = jnp.maximum(run_max, jnp.max(logits, axis=-1))
        probs = jnp.where(allowed, jnp.exp(logits - new_max[..., None]), 0.0)
        factor = jnp.exp(run_max - new_max)
        new_sum = run_sum * factor + jnp.sum(probs, axis=-1)
        new_acc = run_acc * factor[..., None] + jnp.einsum(
            "hqk,khd->hqd", probs, value_piece.astype(jnp.float32)
        )
        return (new_max, new_sum, new_acc)

    def attend(carry, piece, start):
        return lax.cond(
            start > first + block - 1,
            lambda state: state,
            lambda state: update(state, piece, start),
            carry,
        )

    initial = (
        jnp.full((heads, block), -1e30, jnp.float32),
        jnp.zeros((heads, block), jnp.float32),
        jnp.zeros((heads, block, head_size), jnp.float32),
    )
    run_max, run_sum, run_acc = over_all((keys, values), "sp", 0, attend, initial)
    attended = (
        (run_acc / run_sum[..., None]).transpose(1, 0, 2).reshape(block, width).astype(jnp.bfloat16)
    )
    out_full = lax.all_gather(out_weight, "sp", axis=1, tiled=True)
    rows = tokens.shape[0]

    def term(start, count):
        return jnp.dot(
            lax.dynamic_slice_in_dim(attended, start, count, 0),
            out_full,
            preferred_element_type=jnp.float32,
        )

    summed = own_rows(term, rows, "tp")
    normed = summed * lax.rsqrt(jnp.mean(summed * summed, axis=-1, keepdims=True) + 1e-06)
    return (normed * out_gain).astype(jnp.bfloat16)


MESH = pl.DeviceIdType.MESH
Z_, X_, Y_, DA, DB, PC, PX, PY, PA, PB, ZD = range(11)


def rdma(src, dst, send, recv, sp, tp):
    return pltpu.make_async_remote_copy(
        src_ref=src,
        dst_ref=dst,
        send_sem=send,
        recv_sem=recv,
        device_id={"sp": sp, "tp": tp},
        device_id_type=MESH,
    )


class Place:
    def __init__(self, depth):
        sp, tp = lax.axis_index("sp"), lax.axis_index("tp")
        self.depth, self.sp, self.tp = depth, sp, tp
        self.z, self.y = sp // 2, lax.rem(sp, 2)
        self.x, self.c = tp // 2, lax.rem(tp, 2)

    def back(self, j):
        return lax.rem(self.z + self.depth - j, self.depth)

    def ahead(self, j):
        return lax.rem(self.z + j, self.depth)

    def nearest(self, k):
        pick = 0
        for z in range(self.depth):
            others = sorted((abs(o - z), (z - o) % self.depth) for o in range(self.depth))
            pick = pick + jnp.where(self.z == z, others[k][1], 0)
        return pick


class Gather:
    def __init__(self, at, own, buf, send, recv, local, parts):
        self.at, self.own, self.buf = at, own, buf
        self.send, self.recv, self.local = send, recv, local
        self.rows = own.shape[0]
        self.cut = self.rows // parts
        self.sent = []
        self.maybe = []

    def block(self, z, y, x, c, half=None):
        start = (((z * 2 + y) * 2 + x) * 2 + c) * self.rows
        size = self.rows
        if half is not None:
            size = self.rows - self.cut if half else self.cut
            start = start + half * self.cut
        return self.buf.at[pl.ds(pl.multiple_of(start, self.cut), size)]

    def go(self, kind, j, dst, sp, tp, src=None):
        copy = rdma(
            dst if src is None else src,
            dst,
            self.send.at[kind, j],
            self.recv.at[kind, j],
            sp,
            tp,
        )
        copy.start()
        self.sent.append(copy)

    def arrived(self, kind, j, ref):
        pltpu.make_async_copy(ref, ref, self.recv.at[kind, j]).wait()

    def to_x(self, kind, j, ref, src=None):
        a = self.at
        self.go(kind, j, ref, a.sp, (1 - a.x) * 2 + a.c, src)

    def to_y(self, kind, j, ref, src=None):
        a = self.at
        self.go(kind, j, ref, a.z * 2 + 1 - a.y, a.tp, src)

    def to_core(self, kind, j, ref, src=None):
        a = self.at
        self.go(kind, j, ref, a.sp, a.x * 2 + 1 - a.c, src)

    def begin(self):
        a = self.at
        mine = self.block(a.z, a.y, a.x, a.c)
        self.keep = pltpu.make_async_copy(self.own, mine, self.local)
        self.keep.start()
        self.along(a.z < a.depth - 1, Z_, 0, mine, a.ahead(1), 1, self.own)
        self.along(a.z > 0, ZD, 0, mine, a.back(1), a.depth - 1, self.own)
        self.to_core(PC, 0, mine, self.own)

    def spread(self):
        a = self.at
        mine = self.block(a.z, a.y, a.x, a.c)
        self.to_x(X_, 0, mine, self.own)
        self.to_y(Y_, 0, mine, self.own)

    def along(self, when, kind, j, ref, z, k, src=None):
        a = self.at
        copy = rdma(
            ref if src is None else src,
            ref,
            self.send.at[kind, j],
            self.recv.at[Z_, k],
            z * 2 + a.y,
            a.tp,
        )
        self.maybe.append((when, copy))

        @pl.when(when)
        def _():
            copy.start()

    def column(self, j):
        a = self.at
        ref = self.block(a.back(j), a.y, a.x, a.c)
        self.arrived(Z_, j, ref)
        below = j <= a.z
        up = jnp.logical_and(below, a.z < a.depth - 1)
        down = jnp.logical_and(jnp.logical_not(below), a.z > 0)
        self.along(up, Z_, j, ref, a.ahead(1), lax.rem(j + 1, a.depth))
        self.along(down, ZD, j, ref, a.back(1), j - 1)
        self.to_x(X_, j, ref)
        self.to_y(Y_, j, ref)
        self.to_core(PC, j, ref)

    def sides(self, j):
        a = self.at
        z = a.back(j)
        ref = self.block(z, a.y, 1 - a.x, a.c)
        self.arrived(X_, j, ref)
        self.to_y(DA, j, self.block(z, a.y, 1 - a.x, a.c, 0))
        self.to_core(PX, j, ref)
        ref = self.block(z, 1 - a.y, a.x, a.c)
        self.arrived(Y_, j, ref)
        self.to_x(DB, j, self.block(z, 1 - a.y, a.x, a.c, 1))
        self.to_core(PY, j, ref)

    def corner(self, j):
        a = self.at
        z = a.back(j)
        for kind, onward, half in ((DA, PA, 0), (DB, PB, 1)):
            ref = self.block(z, 1 - a.y, 1 - a.x, a.c, half)
            self.arrived(kind, j, ref)
            self.to_core(onward, j, ref)

    def partner(self, j):
        a = self.at
        z, c = a.back(j), 1 - a.c
        self.arrived(PC, j, self.block(z, a.y, a.x, c))
        self.arrived(PX, j, self.block(z, a.y, 1 - a.x, c))
        self.arrived(PY, j, self.block(z, 1 - a.y, a.x, c))
        self.arrived(PA, j, self.block(z, 1 - a.y, 1 - a.x, c, 0))
        self.arrived(PB, j, self.block(z, 1 - a.y, 1 - a.x, c, 1))

    def end(self):
        for copy in self.sent:
            copy.wait_send()
        for when, copy in self.maybe:

            @pl.when(when)
            def _(copy=copy):
                copy.wait_send()


def layer(
    depth, size, tok_ref, q_ref, k_ref, v_ref, g_ref, b_ref, ow_ref, gain_ref, out_ref,
    toks, outw, wq, wkv, gates, bias, keys, vals, cums, cumc, mine, att,
    tok_send, tok_recv, ow_send, ow_recv, w_send, w_recv, p_send, p_recv, a_send, a_recv, keep,
):
    at = Place(depth)
    z, y, x, c = at.z, at.y, at.x, at.c
    home = y == c
    seq = toks.shape[0]
    heads = 4 * depth
    rows = q_ref.shape[0]
    tok = Gather(at, tok_ref, toks, tok_send, tok_recv, keep.at[0], 4)
    ow = Gather(at, ow_ref, outw, ow_send, ow_recv, keep.at[1], 2)

    def w_parts(head, row_block):
        cols = pl.ds(pl.multiple_of(head * size, size), size)
        place = pl.ds(pl.multiple_of(row_block * rows, rows), rows)
        return (
            (q_ref.at[:, cols], wq.at[place]),
            (k_ref.at[:, cols], wkv.at[place, pl.ds(0, size)]),
            (v_ref.at[:, cols], wkv.at[place, pl.ds(size, size)]),
            (g_ref, gates.at[:, place]),
        )

    away = jnp.where(home, 0, 1)

    def send_w(j):
        head = at.ahead(j)
        return [
            rdma(a, b, w_send.at[i, j], w_recv.at[i, j, away], head * 2 + c, at.tp)
            for i, (a, b) in enumerate(w_parts(head, at.sp))
        ]

    def keep_w():
        return [
            pltpu.make_async_copy(a, b, w_recv.at[i, 0, 0])
            for i, (a, b) in enumerate(w_parts(z, at.sp))
        ]

    def pass_w():
        whole = ((wq, wq), (wkv, wkv), (gates, gates), (b_ref, bias))
        return [
            rdma(a, b, p_send.at[i], p_recv.at[i], at.sp, x * 2 + 1 - c)
            for i, (a, b) in enumerate(whole)
        ]

    barrier = pltpu.get_barrier_semaphore()
    near = [(at.sp, x * 2 + 1 - c), (at.sp, (1 - x) * 2 + c), (z * 2 + 1 - y, at.tp)]

    def greet(sp, tp):
        peer = {"sp": sp, "tp": tp}
        pl.semaphore_signal(barrier, inc=1, device_id=peer, device_id_type=MESH)

    for sp, tp in near:
        greet(sp, tp)
    pl.when(z > 0)(lambda: greet(at.sp - 2, at.tp))
    pl.when(z < depth - 1)(lambda: greet(at.sp + 2, at.tp))
    ends = jnp.where(z > 0, 1, 0) + jnp.where(z < depth - 1, 1, 0)
    pl.semaphore_wait(barrier, len(near) + ends)

    tok.begin()
    tok.spread()

    @pl.when(home)
    def _():
        for copy in keep_w():
            copy.start()

    @pl.when(jnp.logical_not(home))
    def _():
        for copy in send_w(0):
            copy.start()

    def later_w(when, j):
        @pl.when(when)
        def _():
            for copy in send_w(depth - j):
                copy.start()

    order = [0] + [at.nearest(k) for k in range(1, depth)]
    for last, j in zip(order[:-1], order[1:]):
        tok.column(j)
        later_w(home, j)
        tok.sides(last)
        if last is not order[0]:
            later_w(jnp.logical_not(home), last)
    ow.begin()
    tok.sides(order[-1])
    later_w(jnp.logical_not(home), order[-1])
    ow.spread()
    tok.corner(order[0])

    @pl.when(home)
    def _():
        for j in range(depth):
            for e in range(2):
                for i, (_a, b) in enumerate(w_parts(z, at.back(j) * 2 + (y if e == 0 else 1 - y))):
                    pltpu.make_async_copy(b, b, w_recv.at[i, j, e]).wait()
        for copy in pass_w():
            copy.start()
        moved = pltpu.make_async_copy(b_ref, bias, keep.at[2])
        moved.start()
        moved.wait()

    for last, j in zip(order[:-1], order[1:]):
        ow.column(j)
        tok.corner(j)
        ow.sides(last)
    tok.keep.wait()
    for j in order:
        tok.partner(j)

    @pl.when(jnp.logical_not(home))
    def _():
        for i, ref in enumerate((wq, wkv, gates, bias)):
            pltpu.make_async_copy(ref, ref, p_recv.at[i]).wait()

    raw = lax.dot_general(
        gates[...], toks[...], (((1,), (1,)), ((), ())), preferred_element_type=jnp.float32
    )[:8]
    raw = raw + bias[:, :1] + math.log(seq)
    run = jnp.minimum(raw, 0.0) - jnp.log1p(jnp.exp(-jnp.abs(raw)))
    lane = lax.broadcasted_iota(jnp.int32, run.shape, 1)
    step = 1
    while step < seq:
        run = run + jnp.where(lane >= step, pltpu.roll(run, step, 1), 0.0)
        step *= 2
    which = lax.broadcasted_iota(jnp.int32, run.shape, 0)
    chosen = jnp.sum(jnp.where(which == z, run, 0.0), axis=0, keepdims=True)
    cums[...] = jnp.broadcast_to(chosen, cums.shape)
    cumc[...] = jnp.broadcast_to(chosen, (128, seq)).T

    span = seq // (2 * depth)
    for i in range(2 * depth):
        part = pl.ds(i * span, span)
        both = jnp.dot(toks[part, :], wkv[...], preferred_element_type=jnp.float32)
        keys[part, :] = both[:, :size].astype(jnp.bfloat16)
        vals[part, :] = both[:, size:].astype(jnp.bfloat16)
    ow.sides(order[-1])

    scale = size ** (-0.5)
    own = span // 4
    head = (2 * x + y) * depth + z

    def deliver(j, dx, dc, local):
        xx = x if dx == 0 else 1 - x
        cc = c if dc == 0 else 1 - c
        start = pl.multiple_of(j * span + (xx * 2 + cc) * own, own)
        src = mine.at[pl.ds(start, own)]
        dst = att.at[:, pl.ds(pl.multiple_of(head * size, size), size)]
        if local:
            return pltpu.make_async_copy(src, dst, a_recv.at[head])
        return rdma(src, dst, a_send.at[j, dx, dc], a_recv.at[head], j * 2 + c, xx * 2 + cc)

    for j in range(depth):
        first = pl.multiple_of((2 * j + c) * span, span)
        length = (2 * j + 2) * span
        queries = jnp.dot(
            toks[pl.ds(first, span), :], wq[...], preferred_element_type=jnp.float32
        ).astype(jnp.bfloat16)
        logits = lax.dot_general(
            queries, keys[:length, :], (((1,), (1,)), ((), ())), preferred_element_type=jnp.float32
        )
        logits = logits * scale + cumc[pl.ds(first, span), :1] - cums[:1, :length]
        key_pos = lax.broadcasted_iota(jnp.int32, logits.shape, 1)
        query_pos = first + lax.broadcasted_iota(jnp.int32, logits.shape, 0)
        logits = jnp.where(key_pos <= query_pos, logits, -1e30)
        probs = jnp.exp(logits - jnp.max(logits, axis=1, keepdims=True))
        total = jnp.sum(probs, axis=1, keepdims=True)
        result = jnp.dot(
            probs.astype(jnp.bfloat16), vals[:length, :], preferred_element_type=jnp.float32
        )
        mine[pl.ds(j * span, span), :] = (result / total).astype(jnp.bfloat16)
        here = jnp.logical_and(home, z == j)
        for dx in range(2):
            for dc in range(2):
                if dx or dc:
                    deliver(j, dx, dc, False).start()

        @pl.when(here)
        def _():
            deliver(j, 0, 0, True).start()

        @pl.when(jnp.logical_not(here))
        def _():
            deliver(j, 0, 0, False).start()

        ow.corner(order[j])

    for j in order:
        ow.partner(j)
    ow.keep.wait()
    for h in range(heads):
        ref = att.at[:, pl.ds(h * size, size)]
        pltpu.make_async_copy(ref, ref, a_recv.at[h]).wait()

    deep, wide = ow_ref.shape
    pieces = []
    for s in range(2 * depth):
        acc = None
        for t in range(4):
            term = jnp.dot(
                att[:, t * deep : (t + 1) * deep],
                outw[(s * 4 + t) * deep : (s * 4 + t + 1) * deep, :],
                preferred_element_type=jnp.float32,
            )
            acc = term if acc is None else acc + term
        pieces.append(acc)
    summed = jnp.concatenate(pieces, axis=1)
    normed = summed * lax.rsqrt(jnp.mean(summed * summed, axis=-1, keepdims=True) + 1e-06)
    out_ref[...] = (normed * gain_ref[...]).astype(jnp.bfloat16)

    tok.end()
    ow.end()
    for j in range(1, depth):
        for copy in send_w(j):
            copy.wait_send()

    @pl.when(jnp.logical_not(home))
    def _():
        for copy in send_w(0):
            copy.wait_send()

    @pl.when(home)
    def _():
        for copy in pass_w():
            copy.wait_send()

    for j in range(depth):
        for dx in range(2):
            for dc in range(2):
                if dx or dc:
                    deliver(j, dx, dc, False).wait_send()

        @pl.when(jnp.logical_not(jnp.logical_and(home, z == j)))
        def _():
            deliver(j, 0, 0, False).wait_send()


def head_per_chip(depth, tokens, qw, kw, vw, gw, fb, ow, gain):
    n_sp, n_tp = lax.axis_size("sp"), lax.axis_size("tp")
    n = n_sp * n_tp
    own, width = tokens.shape
    seq = own * n
    rows = qw.shape[0]
    size = qw.shape[1] // gw.shape[1]
    deep, wide = ow.shape
    gates = jnp.pad(gw.T, ((0, 16 - gw.shape[1]), (0, 0)))
    spread = jnp.broadcast_to(fb[:, None], (fb.shape[0], 128))
    bias = jnp.pad(spread, ((0, 8 - fb.shape[0]), (0, 0)))
    vm = pl.BlockSpec(memory_space=pltpu.VMEM)
    bf, f32 = jnp.bfloat16, jnp.float32
    dma = pltpu.SemaphoreType.DMA
    return pl.pallas_call(
        lambda *refs: layer(depth, size, *refs),
        out_shape=jax.ShapeDtypeStruct((own, wide * n_sp), bf),
        in_specs=[vm] * 8,
        out_specs=vm,
        scratch_shapes=[
            pltpu.VMEM((seq, width), bf),
            pltpu.VMEM((n * deep, wide), bf),
            pltpu.VMEM((rows * n_sp, size), bf),
            pltpu.VMEM((rows * n_sp, 2 * size), bf),
            pltpu.VMEM((16, rows * n_sp), bf),
            pltpu.VMEM((8, 128), f32),
            pltpu.VMEM((seq, size), bf),
            pltpu.VMEM((seq, size), bf),
            pltpu.VMEM((8, seq), f32),
            pltpu.VMEM((seq, 128), f32),
            pltpu.VMEM((seq // 2, size), bf),
            pltpu.VMEM((own, deep * n_tp), bf),
            dma((11, depth)),
            dma((11, depth)),
            dma((11, depth)),
            dma((11, depth)),
            dma((4, depth)),
            dma((4, depth, 2)),
            dma((4,)),
            dma((4,)),
            dma((depth, 2, 2)),
            dma((4 * depth,)),
            dma((3,)),
        ],
        compiler_params=pltpu.CompilerParams(
            collective_id=0, has_side_effects=True, vmem_limit_bytes=60 * 2**20
        ),
        name="layer",
    )(tokens, qw, kw, vw, gates, bias, ow, gain.reshape(1, -1))


def on_any(tokens, qw, kw, vw, gw, fb, ow, gain):
    n_sp, n_tp = lax.axis_size("sp"), lax.axis_size("tp")
    depth = n_sp // 2
    fits = n_sp % 2 == 0 and n_tp == 4 and gw.shape[1] == depth and depth <= 8
    tiles = qw.shape[1] == 128 * depth and qw.shape[0] == 128 and ow.shape[1] % 128 == 0
    if fits and tiles:
        return head_per_chip(depth, tokens, qw, kw, vw, gw, fb, ow, gain)
    return on_device(tokens, qw, kw, vw, gw, fb, ow, gain)


def solution(mesh):
    placed = (
        P(("sp", "tp"), None),
        P("sp", "tp"),
        P("sp", "tp"),
        P("sp", "tp"),
        P("sp", "tp"),
        P("tp"),
        P("tp", "sp"),
        P(),
    )
    return jax.shard_map(
        on_any, mesh=mesh, in_specs=placed, out_specs=P(("sp", "tp"), None), check_vma=False
    )
```
